768 devices in a mesh: row: 24 (over z, core), col: 32 (over y, x).
Axes of the slice: x: 4, y: 8, z: 12, core: 2. Of those that a mesh axis runs over, the one named last changes fastest.
Arguments:
- tokens: bfloat16 [192, 576, 2048], P('row', 'col'), may hold values from -6 to 6
- norm_gain: bfloat16 [2048], replicated, may hold values from 0.099609375 to 1.8984375
- w_in: bfloat16 [2048, 1152], replicated, may hold values from -0.125 to 0.125
- w_out: bfloat16 [1152, 2048], replicated, may hold values from -0.1875 to 0.1875
Outputs:
- mixed: bfloat16 [576, 192, 2048], P('row', 'col')
The draws below stay inside these ranges and needn't reach their ends.
All inputs are finite; a program needn't handle non-finite values.
Results may differ from the reference program's by a relative error of at most 0.013.
Values may be sent and summed in bfloat16 or wider, within the bound.
A program may use at most 64 MiB of HBM per device.

```python
import jax
import jax.numpy as jnp
from jax import lax

D = 2048
GROUP = 128
F = 1152
LEN_A = 192
LEN_B = 576
N_COL = 32


def level_of(stream_key, dims, cuts, low, high):
    level = 1.0
    for axis_at, parts in cuts:
        draws = jax.random.uniform(jax.random.fold_in(jax.random.fold_in(stream_key, 6), axis_at), (parts,), jnp.float32, low / len(cuts), high / len(cuts))
        level = level * jnp.repeat(jnp.exp(draws), dims[axis_at] // parts).reshape((-1,) + (1,) * (len(dims) - 1 - axis_at))
    return level


def gaussian(stream_key, dims, scale, bound, cuts=(), kind=jnp.bfloat16):
    array = scale * jax.random.normal(stream_key, dims, jnp.float32)
    if cuts:
        array = array * level_of(stream_key, dims, cuts, -0.22, 0.18)
    return jnp.clip(array, -bound, bound).astype(kind)


def setup_inputs(seed: int = 0) -> dict:
    arg_keys = jax.random.split(jax.random.key(seed), 5)
    tokens = gaussian(arg_keys[0], (LEN_A, LEN_B, D), 1.0, 6.0, ((0, 24), (1, 32)))
    norm_gain = jnp.clip(1.0 + 0.18 * jax.random.normal(arg_keys[1], (D,), jnp.float32), 0.099609375, 1.8984375).astype(jnp.bfloat16)
    w_in = gaussian(arg_keys[2], (D, F), D ** -0.5, 0.125)
    w_out = gaussian(arg_keys[3], (F, D), F ** -0.5, 0.1875)
    return dict(tokens=tokens, norm_gain=norm_gain, w_in=w_in, w_out=w_out)


norm_eps = 1e-06

def folded_order(length_first, devices):
    block = length_first // devices
    half_block = block // 2
    series = jnp.arange(length_first, dtype=jnp.int32)
    device = series // block
    inner = series % block
    lower = device * half_block + inner
    upper = length_first - device * half_block - (inner - half_block)
    upper = jnp.where((device == 0) & (inner == half_block), length_first // 2, upper)
    return (jnp.where(inner < half_block, lower, upper) % length_first).astype(jnp.int32)

def reference(tokens, norm_gain, w_in, w_out):
    length_first, length_second, features = tokens.shape
    positions = length_first * length_second
    floats = tokens.astype(jnp.float32).reshape(positions, features)
    normed = (floats * lax.rsqrt(lax.optimization_barrier(jnp.mean(floats * floats, axis=-1, keepdims=True)) + norm_eps) * norm_gain.astype(jnp.float32)).astype(jnp.bfloat16)
    mapped = jnp.dot(normed, w_in, preferred_element_type=jnp.float32).astype(jnp.bfloat16)
    channels = mapped.shape[1]
    grouped = mapped.astype(jnp.float32).reshape(positions, channels // GROUP, GROUP).transpose(1, 0, 2)

    def one_group(block):
        return jnp.fft.fft2(block, norm='ortho').real.astype(jnp.float32)
    spectrum = lax.map(one_group, grouped).transpose(1, 0, 2).reshape(positions, channels)
    spectrum = spectrum.astype(jnp.bfloat16)
    mixed = jnp.dot(spectrum, w_out, preferred_element_type=jnp.float32).astype(jnp.bfloat16)
    mixed = mixed.reshape(length_second, length_first, features)
    return jnp.take(mixed, folded_order(length_first, N_COL), axis=1)
```

```python
import math

import jax
import jax.numpy as jnp
import numpy as np
from jax import lax
from jax.experimental import pallas as pl
from jax.experimental.pallas import tpu as pltpu
from jax.sharding import PartitionSpec as P

MESH = pl.DeviceIdType.MESH
F32 = jnp.float32
BF16 = jnp.bfloat16
NORM_EPS = 1e-06

D, GROUP, F = 2048, 128, 1152
LEN_A, LEN_B = 192, 576
NR, NC = 24, 32
GROUPS = F // GROUP
POSITIONS = LEN_A * LEN_B


def host_tables():
    j = np.arange(GROUP)
    lane = np.arange(GROUP)
    q, ch = lane // 16, lane % 16
    m = 8 * q + ch % 8
    sine = ch >= 8
    m = np.where(sine & (m == 0), 64, m)
    sine = sine & (m != 64)
    angle = 2 * np.pi * (j[:, None] * m[None, :] % GROUP) / GROUP
    tc = np.where(sine[None, :], np.sin(angle), np.cos(angle)) / math.sqrt(GROUP)
    fold = np.zeros((GROUP, GROUP))
    fold[lane, m] = 1.0
    pair = (m != 0) & (m != 64)
    fold[lane[pair], GROUP - m[pair]] = np.where(sine[pair], -1.0, 1.0)
    a = np.arange(LEN_A)
    ma = np.zeros((NC, 6, LEN_A))
    for c in range(NC):
        for i in range(3):
            w = 2 * np.pi * (a * (3 * c + i) % LEN_A) / LEN_A
            ma[c, i] = np.cos(w)
            ma[c, 3 + i] = -np.sin(w)
    ma[0, 3] = np.cos(np.pi * a)
    ma = ma.reshape(LEN_A, LEN_A) / math.sqrt(LEN_A)
    lo, hi, r = np.meshgrid(np.arange(8), np.arange(3), np.arange(NR), indexing="ij")
    kb = (24 * r + 8 * hi + lo).reshape(-1)
    bp, cp = np.meshgrid(np.arange(18), np.arange(NC), indexing="ij")
    b = (18 * cp + bp).reshape(-1)
    parts = []
    for k in (kb, LEN_B - 1 - kb):
        w = 2 * np.pi * (k[:, None] * b[None, :] % LEN_B) / LEN_B
        parts.append(np.concatenate([np.cos(w), np.sin(w)], axis=1))
    g = np.concatenate(parts, axis=0) / math.sqrt(LEN_B)
    return [np.asarray(t, dtype=jnp.bfloat16) for t in (tc, ma, g, fold)]


TABLES = host_tables()


def swap8(x):
    lane = lax.broadcasted_iota(jnp.int32, x[0].shape, 1)
    x = list(x)
    for s in (4, 2, 1):
        shift = 16 * s
        bit = (lane & shift) != 0
        for i in range(8):
            if i & s:
                continue
            a, b = x[i], x[i + s]
            x[i] = jnp.where(bit, pltpu.roll(b, shift, 1), a)
            x[i + s] = jnp.where(bit, b, pltpu.roll(a, GROUP - shift, 1))
    return x


def peer_step(k, n):
    k = n - 2 - k
    return jnp.where(k % 2 == 0, 1 + k // 2, n - (k + 1) // 2)


def kernel(
    tok, gain, w_in, w_out, tc_h, ma_h, g_h, fold_h, out,
    xb, gn, xf, xs, wi, wo, wf, tc, ma, gg, fold, mp, tb, s1, r1, zf, s2, r2, f2,
    rr, ii, cs, sn, dd, m3, s3, r3, f3, lh, ls,
    load_sem, send1, recv1, send2, recv2, send3, recv3,
):
    row, col = lax.axis_index("row"), lax.axis_index("col")

    loads = [
        pltpu.make_async_copy(src, dst, load_sem.at[n])
        for n, (src, dst) in enumerate(
            [(tok, xb), (gain, gn), (w_in, wi), (tc_h, tc), (ma_h, ma), (fold_h, fold), (w_out, wo), (g_h, gg)]
        )
    ]
    for load in loads:
        load.start()

    barrier = pltpu.get_barrier_semaphore()

    def greet(k, carry):
        dest = lax.rem(row + 1 + k, NR)
        pl.semaphore_signal(barrier, inc=1, device_id={"row": dest}, device_id_type=MESH)
        return carry

    def greet_col(k, carry):
        dest = lax.rem(col + 1 + k, NC)
        pl.semaphore_signal(barrier, inc=1, device_id={"col": dest}, device_id_type=MESH)
        return carry

    lax.fori_loop(0, NR - 1, greet, 0)
    lax.fori_loop(0, NC - 1, greet_col, 0)

    def send_all(src, dst, ssem, rsem, axis, me, n):
        def one(k, carry):
            dest = lax.rem(me + peer_step(k, n), n)
            pltpu.make_async_remote_copy(
                src.at[dest], dst.at[me], ssem.at[dest], rsem.at[me], device_id={axis: dest}, device_id_type=MESH
            ).start()
            return carry

        lax.fori_loop(0, n - 1, one, 0)

    def wait_all(src, dst, ssem, rsem, axis, me, n, receive):
        def one(k, carry):
            peer = lax.rem(me + 1 + k, n)
            copy = pltpu.make_async_remote_copy(
                src.at[peer], dst.at[peer], ssem.at[peer], rsem.at[peer], device_id={axis: peer}, device_id_type=MESH
            )
            if receive:
                copy.wait_recv()
            else:
                copy.wait_send()
            return carry

        lax.fori_loop(0, n - 1, one, 0)

    loads[0].wait()
    loads[1].wait()

    def norm(a, carry):
        x = xb[a].astype(F32)
        y = x * lax.rsqrt(jnp.mean(x * x, axis=-1, keepdims=True) + NORM_EPS) * gn[...].astype(F32)
        for t in range(D // 128):
            xf[t, pl.ds(pl.multiple_of(24 * a, 8), 18), :] = y[:, 128 * t : 128 * (t + 1)]
        return carry

    lax.fori_loop(0, 8, norm, 0)

    def regroup(n, carry):
        for t in range(D // 128):
            y = jnp.concatenate([xf[t, pl.ds(2 * n, 8, stride=24), :], xf[t, pl.ds(2 * n + 1, 8, stride=24), :]], axis=0)
            xs[pl.ds(pl.multiple_of(16 * n, 16), 16), 128 * t : 128 * (t + 1)] = y.astype(BF16)
        return carry

    lax.fori_loop(0, 9, regroup, 0)
    loads[2].wait()
    loads[3].wait()
    mp[...] = jnp.dot(xs[...], wi[...], preferred_element_type=F32).astype(BF16)
    for g in range(GROUPS):
        values = jnp.dot(mp[:, 128 * g : 128 * (g + 1)], tc[...], preferred_element_type=F32)
        tb[g] = values.reshape(18, 8, GROUP)

    def pack(g, carry):
        o, t = g // 3, g % 3
        for hi in range(2):
            moved = swap8([tb[g, 8 * hi + n] for n in range(8)])
            for q in range(8):
                s1[8 * o + q, 2 * t + hi] = moved[q].astype(BF16)
        return carry

    lax.fori_loop(0, GROUPS, pack, 0)

    def pack_rest(o, carry):
        zero = jnp.zeros((8, GROUP), F32)
        moved = swap8([tb[3 * o + n % 4, 16 + n // 4] if n % 4 < 3 else zero for n in range(8)])
        for q in range(8):
            s1[8 * o + q, 6] = moved[q].astype(BF16)
        return carry

    lax.fori_loop(0, 3, pack_rest, 0)

    pl.semaphore_wait(barrier, NR + NC - 2)
    send_all(s1, r1, send1, recv1, "row", row, NR)
    r1[row] = s1[row]

    shape = (LEN_B, GROUP)
    line = lax.broadcasted_iota(jnp.int32, shape, 0)
    lane = lax.broadcasted_iota(jnp.int32, shape, 1)
    position = (18 * (line & 31) + (line >> 5)).astype(F32)
    sine = ((lane & 8) != 0) & jnp.logical_not((lax.rem(row, 8) == 0) & ((lane & 15) == 8))
    offset = jnp.where(sine, 0.5 * math.pi, 0.0).astype(F32)
    for tile in range(2):
        low = 3 * col + 2 * tile
        high = 3 * col + 1 if tile == 0 else jnp.where(col == 0, LEN_A // 2, 3 * col)
        frequency = jnp.where(lane < 64, low, high).astype(F32)
        angle = position * frequency * (2.0 * math.pi / POSITIONS) + offset
        cs[tile] = jnp.cos(angle)
        sn[tile] = jnp.sin(angle)
    loads[5].wait()
    loads[6].wait()

    def fold_out(g, carry):
        lines = pl.ds(pl.multiple_of(128 * g, 128), 128)
        wf[lines, :] = jnp.dot(fold[...], wo[lines, :], preferred_element_type=F32).astype(BF16)
        return carry

    lax.fori_loop(0, GROUPS, fold_out, 0)
    loads[4].wait()
    loads[7].wait()
    zf[pl.ds(7, LEN_A, stride=8), :] = jnp.zeros((LEN_A, GROUP), F32)
    for n in (54, 55):
        m3[pl.ds(n, NR, stride=56), :] = jnp.zeros((NR, GROUP), F32)

    wait_all(s1, r1, send1, recv1, "row", row, NR, True)
    arrived = jnp.concatenate([r1[:, n].astype(F32).reshape(LEN_A, GROUP) for n in range(7)], axis=1)
    turned = jnp.dot(ma[...], arrived.astype(BF16), preferred_element_type=F32)
    for n in range(7):
        zf[pl.ds(n, LEN_A, stride=8), :] = turned[:, 128 * n : 128 * (n + 1)]
    s2[...] = zf[...].reshape(NC, 48, GROUP).astype(BF16)
    send_all(s2, r2, send2, recv2, "col", col, NC)
    r2[col] = s2[col]
    wait_all(s2, r2, send2, recv2, "col", col, NC, True)

    f2[...] = r2[...].astype(F32).reshape(NC * 48, GROUP)
    inner = (col != 0).astype(F32)
    lane = lax.broadcasted_iota(jnp.int32, (NC, GROUP), 1)
    zero = jnp.zeros((NC, GROUP), F32)

    def part(i, n):
        return f2[pl.ds(8 * i + n, NC, stride=48), :]

    def sets(n):
        i0 = part(3, n)
        i0_kept = i0 * inner
        r0 = part(0, n)
        return ([r0, part(1, n), part(2, n), jnp.where(col == 0, i0, r0)], [i0_kept, part(4, n), part(5, n), i0_kept])

    for hi in range(2):
        by_t = [sets(2 * t + hi) for t in range(3)]
        for kind, target in ((0, rr), (1, ii)):
            for tile in range(2):
                x = []
                for s in (2 * tile, 2 * tile + 1):
                    x += [by_t[t][kind][s] for t in range(3)] + [zero]
                for n, moved in enumerate(swap8(x)):
                    target[tile, 32 * (8 * hi + n) : 32 * (8 * hi + n + 1), :] = moved
    last = sets(6)
    for kind, target in ((0, rr), (1, ii)):
        for tile in range(2):
            x, y = last[kind][2 * tile], last[kind][2 * tile + 1]
            target[tile, 512:544, :] = jnp.where(lane < 64, x, pltpu.roll(y, 64, 1))
            target[tile, 544:576, :] = jnp.where(lane < 64, pltpu.roll(x, 64, 1), y)
    for tile in range(2):
        at = slice(128 * tile, 128 * (tile + 1))
        dd[0:LEN_B, at] = (rr[tile] * cs[tile] + ii[tile] * sn[tile]).astype(BF16)
        dd[LEN_B : 2 * LEN_B, at] = (ii[tile] * cs[tile] - rr[tile] * sn[tile]).astype(BF16)
    lane = lax.broadcasted_iota(jnp.int32, (72, GROUP), 1)
    sine = ((lane & 8) != 0) & jnp.logical_not((lax.rem(row, 8) == 0) & ((lane & 15) == 8))
    sign = jnp.where(sine, -1.0, 1.0).astype(F32)
    for upper in range(2):
        result = jnp.dot(gg[LEN_B * upper : LEN_B * (upper + 1)], dd[...], preferred_element_type=F32)
        for tile in range(2):
            moved = swap8([result[72 * n : 72 * (n + 1), 128 * tile : 128 * (tile + 1)] for n in range(8)])
            for half in range(2):
                s = 2 * tile + half
                i = (s if s < 3 else None) if upper == 0 else (None, 4, 5, 3)[s]
                if i is None:
                    continue
                for t in range(3):
                    values = moved[4 * half + t]
                    if upper:
                        values = values * sign
                    for hi in range(3):
                        m3[pl.ds((3 * i + hi) * 3 + t, NR, stride=56), :] = values[24 * hi : 24 * (hi + 1)]
    s3[...] = m3[...].reshape(NR, 7, 8, GROUP).astype(BF16)
    send_all(s3, r3, send3, recv3, "row", row, NR)
    r3[row] = s3[row]
    wait_all(s3, r3, send3, recv3, "row", row, NR, True)

    f3[...] = r3[...].astype(F32).reshape(NR * 56, GROUP)
    for o in range(3):
        for t in range(3):
            moved = swap8([f3[pl.ds((8 * o + q) * 56 + t, 18, stride=3), :] for q in range(8)])
            for n in range(8):
                lh[3 * o + t, pl.ds(n, 18, stride=8), :] = moved[n]
    for g in range(GROUPS):
        ls[:, 128 * g : 128 * (g + 1)] = lh[g].astype(BF16)

    def project(n, carry):
        at = pl.ds(pl.multiple_of(512 * n, 512), 512)
        out[:, at] = jnp.dot(ls[...], wf[:, at], preferred_element_type=F32).astype(BF16)
        return carry

    lax.fori_loop(0, D // 512, project, 0)

    wait_all(s1, r1, send1, recv1, "row", row, NR, False)
    wait_all(s2, r2, send2, recv2, "col", col, NC, False)
    wait_all(s3, r3, send3, recv3, "row", row, NR, False)


def shards(tokens, norm_gain, w_in, w_out):
    vm = pltpu.VMEM
    dma = pltpu.SemaphoreType.DMA
    out = pl.pallas_call(
        kernel,
        out_shape=jax.ShapeDtypeStruct((144, D), BF16),
        in_specs=[pl.BlockSpec(memory_space=pl.ANY)] * 8,
        out_specs=pl.BlockSpec(memory_space=vm),
        scratch_shapes=[
            vm((8, 18, D), BF16),
            vm((1, D), BF16),
            vm((D // 128, 8 * 24, 128), F32),
            vm((144, D), BF16),
            vm((D, F), BF16),
            vm((F, D), BF16),
            vm((F, D), BF16),
            vm((GROUP, GROUP), BF16),
            vm((LEN_A, LEN_A), BF16),
            vm((2 * LEN_B, 2 * LEN_B), BF16),
            vm((GROUP, GROUP), BF16),
            vm((144, F), BF16),
            vm((GROUPS, 18, 8, GROUP), F32),
            vm((NR, 7, 8, GROUP), BF16),
            vm((NR, 7, 8, GROUP), BF16),
            vm((LEN_A * 8, GROUP), F32),
            vm((NC, 48, GROUP), BF16),
            vm((NC, 48, GROUP), BF16),
            vm((NC * 48, GROUP), F32),
            vm((2, LEN_B, GROUP), F32),
            vm((2, LEN_B, GROUP), F32),
            vm((2, LEN_B, GROUP), F32),
            vm((2, LEN_B, GROUP), F32),
            vm((2 * LEN_B, 2 * GROUP), BF16),
            vm((NR * 56, GROUP), F32),
            vm((NR, 7, 8, GROUP), BF16),
            vm((NR, 7, 8, GROUP), BF16),
            vm((NR * 56, GROUP), F32),
            vm((GROUPS, 144, GROUP), F32),
            vm((144, F), BF16),
            dma((8,)),
            dma((NR,)),
            dma((NR,)),
            dma((NC,)),
            dma((NC,)),
            dma((NR,)),
            dma((NR,)),
        ],
        compiler_params=pltpu.CompilerParams(
            collective_id=0, has_side_effects=True, vmem_limit_bytes=60 * 1024 * 1024
        ),
    )(tokens, norm_gain.reshape(1, D), w_in, w_out, *[jnp.asarray(t) for t in TABLES])
    return out.reshape(6, 3, 8, D).transpose(1, 2, 0, 3).reshape(24, 6, D)


def solution(mesh):
    in_specs = (P("row", "col", None), P(), P(), P())
    out_specs = P("row", "col", None)
    return jax.shard_map(shards, mesh=mesh, in_specs=in_specs, out_specs=out_specs, check_vma=False)
```

```python
import math

import jax
import jax.numpy as jnp
import numpy as np
from jax import lax
from jax.experimental import pallas as pl
from jax.experimental.pallas import tpu as pltpu
from jax.sharding import PartitionSpec as P

MESH = pl.DeviceIdType.MESH
F32 = jnp.float32
BF16 = jnp.bfloat16
NORM_EPS = 1e-06

D, GROUP, F = 2048, 128, 1152
LEN_A, LEN_B = 192, 576
NR, NC = 24, 32
GROUPS = F // GROUP
POSITIONS = LEN_A * LEN_B


def host_tables():
    j = np.arange(GROUP)
    lane = np.arange(GROUP)
    q, ch = lane // 16, lane % 16
    m = 8 * q + ch % 8
    sine = ch >= 8
    m = np.where(sine & (m == 0), 64, m)
    sine = sine & (m != 64)
    angle = 2 * np.pi * (j[:, None] * m[None, :] % GROUP) / GROUP
    tc = np.where(sine[None, :], np.sin(angle), np.cos(angle)) / math.sqrt(GROUP)
    fold = np.zeros((GROUP, GROUP))
    fold[lane, m] = 1.0
    pair = (m != 0) & (m != 64)
    fold[lane[pair], GROUP - m[pair]] = np.where(sine[pair], -1.0, 1.0)
    a = np.arange(LEN_A)
    ma = np.zeros((NC, 8, LEN_A))
    for c in range(NC):
        for i in range(3):
            w = 2 * np.pi * (a * (3 * c + i) % LEN_A) / LEN_A
            ma[c, i] = np.cos(w)
            ma[c, 3 + i] = -np.sin(w)
    ma[0, 3] = np.cos(np.pi * a)
    ma = ma.reshape(NC * 8, LEN_A) / math.sqrt(LEN_A)
    lo, hi, r = np.meshgrid(np.arange(8), np.arange(3), np.arange(NR), indexing="ij")
    kb = (24 * r + 8 * hi + lo).reshape(-1)
    bp, cp = np.meshgrid(np.arange(18), np.arange(NC), indexing="ij")
    b = (18 * cp + bp).reshape(-1)
    w = 2 * np.pi * (kb[:, None] * b[None, :] % LEN_B) / LEN_B
    g = np.concatenate([np.cos(w), np.sin(w)], axis=1) / math.sqrt(LEN_B)
    return [np.asarray(t, dtype=jnp.bfloat16) for t in (tc, ma, g, fold)]


TABLES = host_tables()
TILES1 = ((0, 3), (3, 5), (5, 7))
TILES3 = ((0, 2), (2, 4), (4, 7))


def swap8(x):
    lane = lax.broadcasted_iota(jnp.int32, x[0].shape, 1)
    x = list(x)
    for s in (4, 2, 1):
        shift = 16 * s
        bit = (lane & shift) != 0
        for i in range(8):
            if i & s:
                continue
            a, b = x[i], x[i + s]
            x[i] = jnp.where(bit, pltpu.roll(b, shift, 1), a)
            x[i + s] = jnp.where(bit, b, pltpu.roll(a, GROUP - shift, 1))
    return x


def peer_step(k, n):
    k = n - 2 - k
    return jnp.where(k % 2 == 0, 1 + k // 2, n - (k + 1) // 2)


def kernel(
    tok, gain, w_in, w_out, tc_h, ma_h, g_h, fold_h, out,
    xb, gn, xs, wi, wo, wf, tc, ma, gg, fold, mp, tb, s1, r1, za, zb, sa, ra, sb, rb, fa, fb,
    rr, ii, cs, sn, dd, m3, s3, r3, f3, lh, acc,
    load_sem, send1, recv1, send2, recv2, send3, recv3,
):
    row, col = lax.axis_index("row"), lax.axis_index("col")

    loads = [
        pltpu.make_async_copy(src, dst, load_sem.at[n])
        for n, (src, dst) in enumerate(
            [(tok, xb), (gain, gn), (w_in, wi), (tc_h, tc), (ma_h, ma), (fold_h, fold), (w_out, wo), (g_h, gg)]
        )
    ]
    for load in loads:
        load.start()

    barrier = pltpu.get_barrier_semaphore()

    def greet(k, carry):
        dest = lax.rem(row + 1 + k, NR)
        pl.semaphore_signal(barrier, inc=1, device_id={"row": dest}, device_id_type=MESH)
        return carry

    def greet_col(k, carry):
        dest = lax.rem(col + 1 + k, NC)
        pl.semaphore_signal(barrier, inc=1, device_id={"col": dest}, device_id_type=MESH)
        return carry

    lax.fori_loop(0, NR - 1, greet, 0)
    lax.fori_loop(0, NC - 1, greet_col, 0)

    def send_all(src, dst, ssem, rsem, axis, me, n, first, last):
        tiles = pl.ds(first, last - first)

        def one(k, carry):
            dest = lax.rem(me + peer_step(k, n), n)
            pltpu.make_async_remote_copy(
                src.at[dest, tiles], dst.at[me, tiles], ssem, rsem, device_id={axis: dest}, device_id_type=MESH
            ).start()
            return carry

        lax.fori_loop(0, n - 1, one, 0)
        dst[me, first:last] = src[me, first:last]

    def wait_all(buffer, sem, n, first, last):
        part = buffer.at[pl.ds(0, n - 1), pl.ds(first, last - first)]
        pltpu.make_async_copy(part, part, sem).wait()

    loads[0].wait()
    loads[1].wait()
    scale = gn[...].astype(F32).reshape(1, D)

    def norm(n, carry):
        x = xb[pl.ds(2 * n, 2)].astype(F32).reshape(16, D)
        y = x * lax.rsqrt(jnp.mean(x * x, axis=-1, keepdims=True) + NORM_EPS) * scale
        xs[pl.ds(pl.multiple_of(16 * n, 16), 16), :] = y.astype(BF16)
        return carry

    lax.fori_loop(0, 9, norm, 0)
    loads[2].wait()
    loads[3].wait()
    mp[...] = jnp.dot(xs[...], wi[...], preferred_element_type=F32).astype(BF16)
    for g in range(GROUPS):
        o, t = g // 3, g % 3
        values = jnp.dot(mp[:, 128 * g : 128 * (g + 1)], tc[...], preferred_element_type=F32)
        tb[t, :, 8 * o : 8 * (o + 1), :] = values.reshape(18, 8, GROUP)

    def place(moved, tile):
        for q in range(8):
            for o in range(3):
                s1[8 * o + q, tile] = moved[q][8 * o : 8 * (o + 1)].astype(BF16)

    for t in range(3):
        first, last = TILES1[t]
        for hi in range(2):
            place(swap8([tb[t, 8 * hi + n] for n in range(8)]), first + hi)
        if t == 0:
            zero = jnp.zeros((24, GROUP), F32)
            place(swap8([tb[n % 4, 16 + n // 4] if n % 4 < 3 else zero for n in range(8)]), 2)
            pl.semaphore_wait(barrier, NR + NC - 2)
        send_all(s1, r1, send1.at[t], recv1.at[t], "row", row, NR, first, last)

    shape = (LEN_B, GROUP)
    line = lax.broadcasted_iota(jnp.int32, shape, 0)
    lane = lax.broadcasted_iota(jnp.int32, shape, 1)
    position = (18 * (line & 31) + (line >> 5)).astype(F32)
    sine = ((lane & 8) != 0) & jnp.logical_not((lax.rem(row, 8) == 0) & ((lane & 15) == 8))
    offset = jnp.where(sine, 0.5 * math.pi, 0.0).astype(F32)
    i = lane >> 4
    frequency = jnp.where(i < 3, 3 * col + i, LEN_A - (3 * col + i - 3))
    frequency = jnp.where((i == 3) & (col == 0), LEN_A // 2, frequency).astype(F32)
    angle = position * frequency * (2.0 * math.pi / POSITIONS) + offset
    cs[...] = jnp.cos(angle)
    sn[...] = jnp.sin(angle)
    loads[4].wait()
    za[pl.ds(3, 8 * NC, stride=4), :] = jnp.zeros((8 * NC, GROUP), F32)
    for n in (54, 55):
        m3[pl.ds(n, NR, stride=56), :] = jnp.zeros((NR, GROUP), F32)

    for t in range(3):
        first, last = TILES1[t]
        wait_all(r1, recv1.at[t], NR, first, last)
        arrived = [r1[:, n].astype(F32).reshape(LEN_A, GROUP) for n in range(first, last)]
        arrived = jnp.concatenate(arrived, axis=1).astype(BF16)
        turned = jnp.dot(ma[...], arrived, preferred_element_type=F32)
        if t == 0:
            for n in range(3):
                za[pl.ds(n, 8 * NC, stride=4), :] = turned[:, 128 * n : 128 * (n + 1)]
            sa[...] = za[...].reshape(NC, 4, 8, GROUP).astype(BF16)
            send_all(sa, ra, send2.at[t], recv2.at[t], "col", col, NC, 0, 3)
        else:
            for n in range(2):
                zb[pl.ds(n, 8 * NC, stride=2), :] = turned[:, 128 * n : 128 * (n + 1)]
            sb[t - 1] = zb[...].reshape(NC, 2, 8, GROUP).astype(BF16)
            send_all(sb.at[t - 1], rb.at[t - 1], send2.at[t], recv2.at[t], "col", col, NC, 0, 2)

    loads[5].wait()
    loads[6].wait()
    for t in range(3):
        for o in range(3):
            source, target = 128 * (3 * o + t), 128 * (3 * t + o)
            wf[target : target + 128, :] = jnp.dot(
                fold[...], wo[source : source + 128, :], preferred_element_type=F32
            ).astype(BF16)
    loads[7].wait()

    inner = (col != 0).astype(F32)
    zero = jnp.zeros((NC, GROUP), F32)

    def spread(part):
        r0, r1_, r2_, i0, i1, i2 = [part(n) for n in range(6)]
        mirrored = jnp.where(col == 0, i0, r0)
        i0 = i0 * inner
        real = swap8([r0, r1_, r2_, mirrored, r1_, r2_, zero, zero])
        imag = swap8([i0, i1, i2, -i0, -i1, -i2, zero, zero])
        return real, imag

    for t in range(3):
        if t == 0:
            wait_all(ra, recv2.at[t], NC, 0, 3)
            fa[...] = ra[...].astype(F32).reshape(NC * 24, GROUP)
            real, imag = spread(lambda n: fa[pl.ds(4 * n + 2, NC, stride=24), :])
            for b2 in range(2):
                at = slice(32 * (16 + b2), 32 * (17 + b2))
                for u in range(3):
                    rr[u, at, :] = real[4 * b2 + u]
                    ii[u, at, :] = imag[4 * b2 + u]
        else:
            wait_all(rb.at[t - 1], recv2.at[t], NC, 0, 2)
            fb[...] = rb[t - 1].astype(F32).reshape(NC * 16, GROUP)
        for hi in range(2):
            if t == 0:
                real, imag = spread(lambda n: fa[pl.ds(4 * n + hi, NC, stride=24), :])
            else:
                real, imag = spread(lambda n: fb[pl.ds(2 * n + hi, NC, stride=16), :])
            for n in range(8):
                at = slice(32 * (8 * hi + n), 32 * (8 * hi + n + 1))
                rr[t, at, :] = real[n]
                ii[t, at, :] = imag[n]
        dd[0:LEN_B, :] = (rr[t] * cs[...] + ii[t] * sn[...]).astype(BF16)
        dd[LEN_B : 2 * LEN_B, :] = (ii[t] * cs[...] - rr[t] * sn[...]).astype(BF16)
        result = jnp.dot(gg[...], dd[...], preferred_element_type=F32)
        moved = swap8([result[72 * n : 72 * (n + 1)] for n in range(8)])
        for i in range(6):
            for hi in range(3):
                m3[pl.ds(18 * t + 3 * i + hi, NR, stride=56), :] = moved[i][24 * hi : 24 * (hi + 1)]
        first, last = TILES3[t]
        s3[:, first:last] = m3.reshape(NR, 7, 8, GROUP)[:, first:last].astype(BF16)
        send_all(s3, r3, send3.at[t], recv3.at[t], "row", row, NR, first, last)

    def take(first, last):
        f3.reshape(NR, 7, 8, GROUP)[:, first:last] = r3[:, first:last].astype(F32)

    def project(t, last):
        for o in range(3):
            moved = swap8([f3[pl.ds((8 * o + q) * 56 + 18 * t, 18), :] for q in range(8)])
            for n in range(8):
                lh[o, pl.ds(n, 18, stride=8), :] = moved[n]
        values = jnp.concatenate([lh[o] for o in range(3)], axis=1).astype(BF16)
        for n in range(D // 512):
            at = slice(512 * n, 512 * (n + 1))
            part = jnp.dot(values, wf[384 * t : 384 * (t + 1), at], preferred_element_type=F32)
            if t:
                part = part + acc[:, at]
            if last:
                out[:, at] = part.astype(BF16)
            else:
                acc[:, at] = part

    wait_all(r3, recv3.at[0], NR, *TILES3[0])
    wait_all(r3, recv3.at[1], NR, *TILES3[1])
    take(0, 4)
    project(0, False)
    wait_all(r3, recv3.at[2], NR, *TILES3[2])
    take(4, 7)
    project(1, False)
    project(2, True)

    for t in range(3):
        wait_all(s1, send1.at[t], NR, *TILES1[t])
        if t == 0:
            wait_all(sa, send2.at[t], NC, 0, 3)
        else:
            wait_all(sb.at[t - 1], send2.at[t], NC, 0, 2)
        wait_all(s3, send3.at[t], NR, *TILES3[t])


def shards(tokens, norm_gain, w_in, w_out):
    vm = pltpu.VMEM
    dma = pltpu.SemaphoreType.DMA
    out = pl.pallas_call(
        kernel,
        out_shape=jax.ShapeDtypeStruct((144, D), BF16),
        in_specs=[pl.BlockSpec(memory_space=pl.ANY)] * 8,
        out_specs=pl.BlockSpec(memory_space=vm),
        scratch_shapes=[
            vm((18, 8, D), BF16),
            vm((D,), BF16),
            vm((144, D), BF16),
            vm((D, F), BF16),
            vm((F, D), BF16),
            vm((F, D), BF16),
            vm((GROUP, GROUP), BF16),
            vm((8 * NC, LEN_A), BF16),
            vm((LEN_B, 2 * LEN_B), BF16),
            vm((GROUP, GROUP), BF16),
            vm((144, F), BF16),
            vm((3, 18, 24, GROUP), F32),
            vm((NR, 7, 8, GROUP), BF16),
            vm((NR, 7, 8, GROUP), BF16),
            vm((NC * 32, GROUP), F32),
            vm((NC * 16, GROUP), F32),
            vm((NC, 4, 8, GROUP), BF16),
            vm((NC, 3, 8, GROUP), BF16),
            vm((2, NC, 2, 8, GROUP), BF16),
            vm((2, NC, 2, 8, GROUP), BF16),
            vm((NC * 24, GROUP), F32),
            vm((NC * 16, GROUP), F32),
            vm((3, LEN_B, GROUP), F32),
            vm((3, LEN_B, GROUP), F32),
            vm((LEN_B, GROUP), F32),
            vm((LEN_B, GROUP), F32),
            vm((2 * LEN_B, GROUP), BF16),
            vm((NR * 56, GROUP), F32),
            vm((NR, 7, 8, GROUP), BF16),
            vm((NR, 7, 8, GROUP), BF16),
            vm((NR * 56, GROUP), F32),
            vm((3, 144, GROUP), F32),
            vm((144, D), F32),
            dma((8,)),
            dma((3,)),
            dma((3,)),
            dma((3,)),
            dma((3,)),
            dma((3,)),
            dma((3,)),
        ],
        compiler_params=pltpu.CompilerParams(
            collective_id=0, has_side_effects=True, vmem_limit_bytes=60 * 1024 * 1024
        ),
    )(tokens.transpose(1, 0, 2), norm_gain, w_in, w_out, *[jnp.asarray(t) for t in TABLES])
    return out.reshape(6, 3, 8, D).transpose(1, 2, 0, 3).reshape(24, 6, D)


def solution(mesh):
    in_specs = (P("row", "col", None), P(), P(), P())
    out_specs = P("row", "col", None)
    return jax.shard_map(shards, mesh=mesh, in_specs=in_specs, out_specs=out_specs, check_vma=False)
```

```python
import math

import jax
import jax.numpy as jnp
import numpy as np
from jax import lax
from jax.experimental import pallas as pl
from jax.experimental.pallas import tpu as pltpu
from jax.sharding import PartitionSpec as P

MESH = pl.DeviceIdType.MESH
F32 = jnp.float32
BF16 = jnp.bfloat16
NORM_EPS = 1e-06

D, GROUP, F = 2048, 128, 1152
LEN_A, LEN_B = 192, 576
NR, NC = 24, 32
GROUPS = F // GROUP
POSITIONS = LEN_A * LEN_B


def host_tables():
    j = np.arange(GROUP)
    lane = np.arange(GROUP)
    q, ch = lane // 16, lane % 16
    m = 8 * q + ch % 8
    sine = ch >= 8
    m = np.where(sine & (m == 0), 64, m)
    sine = sine & (m != 64)
    angle = 2 * np.pi * (j[:, None] * m[None, :] % GROUP) / GROUP
    tc = np.where(sine[None, :], np.sin(angle), np.cos(angle)) / math.sqrt(GROUP)
    fold = np.zeros((GROUP, GROUP))
    fold[lane, m] = 1.0
    pair = (m != 0) & (m != 64)
    fold[lane[pair], GROUP - m[pair]] = np.where(sine[pair], -1.0, 1.0)
    a = np.arange(LEN_A)
    ma = np.zeros((NC, 8, LEN_A))
    for c in range(NC):
        for i in range(3):
            w = 2 * np.pi * (a * (3 * c + i) % LEN_A) / LEN_A
            ma[c, i] = np.cos(w)
            ma[c, 3 + i] = -np.sin(w)
    ma[0, 3] = np.cos(np.pi * a)
    ma = ma.reshape(NC * 8, LEN_A) / math.sqrt(LEN_A)
    lo, hi, r = np.meshgrid(np.arange(8), np.arange(3), np.arange(NR), indexing="ij")
    kb = (24 * r + 8 * hi + lo).reshape(-1)
    bp, cp = np.meshgrid(np.arange(18), np.arange(NC), indexing="ij")
    b = (18 * cp + bp).reshape(-1)
    w = 2 * np.pi * (kb[:, None] * b[None, :] % LEN_B) / LEN_B
    g = np.concatenate([np.cos(w), np.sin(w)], axis=1) / math.sqrt(LEN_B)
    small = np.zeros((8 * NC, 2 * LEN_B))
    small[:, :LEN_A] = ma
    small[:GROUP, 256:384] = tc
    small[:GROUP, 384:512] = fold
    return np.asarray(np.concatenate([g, small]), dtype=jnp.bfloat16)


TABLE = host_tables()
TILES1 = ((0, 3), (3, 5), (5, 7))
TILES3 = ((0, 2), (2, 4), (4, 7))


def swap8(x):
    lane = lax.broadcasted_iota(jnp.int32, x[0].shape, 1)
    x = list(x)
    for s in (4, 2, 1):
        shift = 16 * s
        bit = (lane & shift) != 0
        for i in range(8):
            if i & s:
                continue
            a, b = x[i], x[i + s]
            x[i] = jnp.where(bit, pltpu.roll(b, shift, 1), a)
            x[i + s] = jnp.where(bit, b, pltpu.roll(a, GROUP - shift, 1))
    return x


def kernel(
    tok, gain, w_in, w_out, table, out,
    xb, gn, xs, wi, wo, wf, small, gg, ma, mp, tb, s1, r1, zr, zb, sb, rb, fb,
    rr, ii, cs, sn, dd, m3, s3, r3, f3, lh, acc,
    load_sem, send1, recv1, send2, recv2, send3, recv3,
):
    row, col = lax.axis_index("row"), lax.axis_index("col")

    loads = [
        pltpu.make_async_copy(src, dst, load_sem.at[n])
        for n, (src, dst) in enumerate(
            [
                (tok, xb),
                (gain, gn),
                *[(w_in.at[pl.ds(512 * k, 512)], wi.at[pl.ds(512 * k, 512)]) for k in range(4)],
                (table.at[LEN_B:, 0:512], small),
                (table.at[0:LEN_B], gg),
                (w_out, wo),
            ]
        )
    ]
    for load in loads[:7]:
        load.start()

    barrier = pltpu.get_barrier_semaphore()

    def both_ways(me, n, act):
        act(jnp.where(me >= n // 2, me - n // 2, me + n // 2))

        def one(k, carry):
            d = n // 2 - 1 - k
            up, down = me + d, me - d
            act(jnp.where(up >= n, up - n, up))
            act(jnp.where(down < 0, down + n, down))
            return carry

        lax.fori_loop(0, n // 2 - 1, one, 0)

    def greet(axis):
        return lambda peer: pl.semaphore_signal(barrier, inc=1, device_id={axis: peer}, device_id_type=MESH)

    both_ways(row, NR, greet("row"))
    both_ways(col, NC, greet("col"))

    def send_all(src, dst, ssem, rsem, axis, me, n, first, last):
        tiles = pl.ds(first, last - first)

        def one(dest):
            pltpu.make_async_remote_copy(
                src.at[dest, tiles], dst.at[me, tiles], ssem, rsem, device_id={axis: dest}, device_id_type=MESH
            ).start()

        both_ways(me, n, one)
        dst[me, first:last] = src[me, first:last]

    def wait_all(buffer, sem, n, first, last):
        part = buffer.at[pl.ds(0, n - 1), pl.ds(first, last - first)]
        pltpu.make_async_copy(part, part, sem).wait()

    loads[0].wait()
    loads[1].wait()
    scale = gn[...].astype(F32).reshape(1, D)

    def norm(n, carry):
        x = xb[pl.ds(2 * n, 2)].astype(F32).reshape(16, D)
        y = x * lax.rsqrt(jnp.mean(x * x, axis=-1, keepdims=True) + NORM_EPS) * scale
        xs[pl.ds(pl.multiple_of(16 * n, 16), 16), :] = y.astype(BF16)
        return carry

    lax.fori_loop(0, 9, norm, 0, unroll=True)
    for k in range(4):
        at = slice(512 * k, 512 * (k + 1))
        loads[2 + k].wait()
        part = jnp.dot(xs[:, at], wi[at, :], preferred_element_type=F32)
        if k:
            part = part + ma[...]
        if k < 3:
            ma[...] = part
        else:
            mp[...] = part.astype(BF16)
    loads[6].wait()
    loads[7].start()
    loads[8].start()
    for g in range(GROUPS):
        o, t = g // 3, g % 3
        values = jnp.dot(mp[:, 128 * g : 128 * (g + 1)], small[0:GROUP, 256:384], preferred_element_type=F32)
        tb[t, :, 8 * o : 8 * (o + 1), :] = values.reshape(18, 8, GROUP)

    def place(moved, tile):
        for q in range(8):
            for o in range(3):
                s1[8 * o + q, tile] = moved[q][8 * o : 8 * (o + 1)].astype(BF16)

    for t in range(3):
        first, last = TILES1[t]
        for hi in range(2):
            place(swap8([tb[t, 8 * hi + n] for n in range(8)]), first + hi)
        if t == 0:
            zero = jnp.zeros((24, GROUP), F32)
            place(swap8([tb[n // 2, 16 + n % 2] if n < 6 else zero for n in range(8)]), 2)
            pl.semaphore_wait(barrier, NR + NC - 2)
        send_all(s1, r1, send1.at[t], recv1.at[t], "row", row, NR, first, last)

    shape = (LEN_B, GROUP)
    line = lax.broadcasted_iota(jnp.int32, shape, 0)
    lane = lax.broadcasted_iota(jnp.int32, shape, 1)
    position = (18 * (line & 31) + (line >> 5)).astype(F32)
    sine = ((lane & 8) != 0) & jnp.logical_not((lax.rem(row, 8) == 0) & ((lane & 15) == 8))
    offset = jnp.where(sine, 0.5 * math.pi, 0.0).astype(F32)
    i = lane >> 4
    frequency = jnp.where(i < 3, 3 * col + i, LEN_A - (3 * col + i - 3))
    frequency = jnp.where((i == 3) & (col == 0), LEN_A // 2, frequency).astype(F32)
    angle = position * frequency * (2.0 * math.pi / POSITIONS) + offset
    cs[...] = jnp.cos(angle)
    sn[...] = jnp.sin(angle)
    for n in (54, 55):
        m3[pl.ds(n, NR, stride=56), :] = jnp.zeros((NR, GROUP), F32)

    def turn(x, shift):
        return pltpu.roll(x, shift % GROUP, 1) if shift % GROUP else x

    for t in range(3):
        first, last = TILES1[t]
        wait_all(r1, recv1.at[t], NR, first, last)
        arrived = [r1[:, n].astype(F32).reshape(LEN_A, GROUP) for n in range(first, last)]
        arrived = jnp.concatenate(arrived, axis=1).astype(BF16)
        turned = jnp.dot(small[:, 0:LEN_A], arrived, preferred_element_type=F32)
        for n in range(2):
            zb[pl.ds(n, 8 * NC, stride=2), :] = turned[:, 128 * n : 128 * (n + 1)]
        if t == 0:
            zr[...] = turned[:, 256:384]
        left = [zr[pl.ds(n, NC, stride=8), :] for n in range(6)]
        block = lax.broadcasted_iota(jnp.int32, (NC, GROUP), 1) >> 5
        for half, slots in ((0, (0, 1, 2, 3)), (1, (4, 5))):
            line = jnp.zeros((NC, GROUP), F32)
            for n in slots:
                line = jnp.where(block == n % 4, turn(left[n], 32 * (n % 4 - t)), line)
            zb[pl.ds(12 + half, NC, stride=16), :] = line
        sb[t] = zb[...].reshape(NC, 2, 8, GROUP).astype(BF16)
        send_all(sb.at[t], rb.at[t], send2.at[t], recv2.at[t], "col", col, NC, 0, 2)

    loads[7].wait()

    inner = (col != 0).astype(F32)
    zero = jnp.zeros((NC, GROUP), F32)

    def spread(part):
        r0, r1_, r2_, i0, i1, i2 = [part(n) for n in range(6)]
        mirrored = jnp.where(col == 0, i0, r0)
        i0 = i0 * inner
        real = swap8([r0, r1_, r2_, mirrored, r1_, r2_, zero, zero])
        imag = swap8([i0, i1, i2, -i0, -i1, -i2, zero, zero])
        return real, imag

    granule = lax.broadcasted_iota(jnp.int32, (NC, GROUP), 1) >> 4

    def gather(picks):
        tile = zero
        for n, (x, k, f) in enumerate(picks):
            value = turn(x, 16 * (n - k))
            tile = jnp.where(granule == n, value if f is None else value * f, tile)
        return tile

    for t in range(3):
        wait_all(rb.at[t], recv2.at[t], NC, 0, 2)
        fb[...] = rb[t].astype(F32).reshape(NC * 16, GROUP)
        x, y = fb[pl.ds(12, NC, stride=16), :], fb[pl.ds(13, NC, stride=16), :]
        for b2 in range(2):
            at = slice(32 * (16 + b2), 32 * (17 + b2))
            i0, i1, i2 = (x, 6 + b2), (y, b2), (y, 2 + b2)
            r0, r1_, r2_ = [(x, 2 * n + b2, None) for n in range(3)]
            tile = gather([r0, r1_, r2_, r0, r1_, r2_])
            rr[t, at, :] = jnp.where((granule == 3) & (col == 0), turn(x, 16 * (3 - i0[1])), tile)
            ii[t, at, :] = gather(
                [(*i0, inner), (*i1, None), (*i2, None), (*i0, -inner), (*i1, -1.0), (*i2, -1.0)]
            )
        for hi in range(2):
            real, imag = spread(lambda n: fb[pl.ds(2 * n + hi, NC, stride=16), :])
            for n in range(8):
                at = slice(32 * (8 * hi + n), 32 * (8 * hi + n + 1))
                rr[t, at, :] = real[n]
                ii[t, at, :] = imag[n]
        dd[0:LEN_B, :] = (rr[t] * cs[...] + ii[t] * sn[...]).astype(BF16)
        dd[LEN_B : 2 * LEN_B, :] = (ii[t] * cs[...] - rr[t] * sn[...]).astype(BF16)
        result = jnp.dot(gg[...], dd[...], preferred_element_type=F32)
        moved = swap8([result[72 * n : 72 * (n + 1)] for n in range(8)])
        for i in range(6):
            for hi in range(3):
                m3[pl.ds(18 * t + 3 * i + hi, NR, stride=56), :] = moved[i][24 * hi : 24 * (hi + 1)]
        first, last = TILES3[t]
        s3[:, first:last] = m3.reshape(NR, 7, 8, GROUP)[:, first:last].astype(BF16)
        send_all(s3, r3, send3.at[t], recv3.at[t], "row", row, NR, first, last)

    def take(first, last):
        f3.reshape(NR, 7, 8, GROUP)[:, first:last] = r3[:, first:last].astype(F32)

    def project(t, last):
        for o in range(3):
            moved = swap8([f3[pl.ds((8 * o + q) * 56 + 18 * t, 18), :] for q in range(8)])
            for n in range(8):
                lh[o, pl.ds(n, 18, stride=8), :] = moved[n]
        values = jnp.concatenate([lh[o] for o in range(3)], axis=1).astype(BF16)
        for n in range(D // 512):
            at = slice(512 * n, 512 * (n + 1))
            part = jnp.dot(values, wf[384 * t : 384 * (t + 1), at], preferred_element_type=F32)
            if t:
                part = part + acc[:, at]
            if last:
                out[:, at] = part.astype(BF16)
            else:
                acc[:, at] = part

    loads[8].wait()
    for t in range(3):
        for o in range(3):
            source, target = 128 * (3 * o + t), 128 * (3 * t + o)
            wf[target : target + 128, :] = jnp.dot(
                small[0:GROUP, 384:512], wo[source : source + 128, :], preferred_element_type=F32
            ).astype(BF16)
    wait_all(r3, recv3.at[0], NR, *TILES3[0])
    wait_all(r3, recv3.at[1], NR, *TILES3[1])
    take(0, 4)
    project(0, False)
    wait_all(r3, recv3.at[2], NR, *TILES3[2])
    take(4, 7)
    project(1, False)
    project(2, True)

    for t in range(3):
        wait_all(s1, send1.at[t], NR, *TILES1[t])
        wait_all(sb.at[t], send2.at[t], NC, 0, 2)
        wait_all(s3, send3.at[t], NR, *TILES3[t])


def shards(tokens, norm_gain, w_in, w_out):
    vm = pltpu.VMEM
    dma = pltpu.SemaphoreType.DMA
    operands = tokens.transpose(1, 0, 2), norm_gain, w_in, w_out, jnp.asarray(TABLE)
    out = pl.pallas_call(
        kernel,
        out_shape=jax.ShapeDtypeStruct((144, D), BF16),
        in_specs=[pl.BlockSpec(memory_space=pl.ANY)] * 5,
        out_specs=pl.BlockSpec(memory_space=vm),
        scratch_shapes=[
            vm((18, 8, D), BF16),
            vm((D,), BF16),
            vm((144, D), BF16),
            vm((D, F), BF16),
            vm((F, D), BF16),
            vm((F, D), BF16),
            vm((8 * NC, 512), BF16),
            vm((LEN_B, 2 * LEN_B), BF16),
            vm((144, F), F32),
            vm((144, F), BF16),
            vm((3, 18, 24, GROUP), F32),
            vm((NR, 7, 8, GROUP), BF16),
            vm((NR, 7, 8, GROUP), BF16),
            vm((NC * 8, GROUP), F32),
            vm((NC * 16, GROUP), F32),
            vm((3, NC, 2, 8, GROUP), BF16),
            vm((3, NC, 2, 8, GROUP), BF16),
            vm((NC * 16, GROUP), F32),
            vm((3, LEN_B, GROUP), F32),
            vm((3, LEN_B, GROUP), F32),
            vm((LEN_B, GROUP), F32),
            vm((LEN_B, GROUP), F32),
            vm((2 * LEN_B, GROUP), BF16),
            vm((NR * 56, GROUP), F32),
            vm((NR, 7, 8, GROUP), BF16),
            vm((NR, 7, 8, GROUP), BF16),
            vm((NR * 56, GROUP), F32),
            vm((3, 144, GROUP), F32),
            vm((144, D), F32),
            dma((9,)),
            dma((3,)),
            dma((3,)),
            dma((3,)),
            dma((3,)),
            dma((3,)),
            dma((3,)),
        ],
        compiler_params=pltpu.CompilerParams(
            collective_id=0, has_side_effects=True, vmem_limit_bytes=50 * 1024 * 1024
        ),
    )(*[pltpu.with_memory_space_constraint(x, pltpu.HBM) for x in operands])
    return out.reshape(6, 3, 8, D).transpose(1, 2, 0, 3).reshape(24, 6, D)


def solution(mesh):
    in_specs = (P("row", "col", None), P(), P(), P())
    out_specs = P("row", "col", None)
    return jax.shard_map(shards, mesh=mesh, in_specs=in_specs, out_specs=out_specs, check_vma=False)
```

```python
import math

import jax
import jax.numpy as jnp
import numpy as np
from jax import lax
from jax.experimental import pallas as pl
from jax.experimental.pallas import tpu as pltpu
from jax.sharding import PartitionSpec as P

MESH = pl.DeviceIdType.MESH
F32 = jnp.float32
BF16 = jnp.bfloat16
NORM_EPS = 1e-06

D, GROUP, F = 2048, 128, 1152
LEN_A, LEN_B = 192, 576
NR, NC = 24, 32
GROUPS = F // GROUP
POSITIONS = LEN_A * LEN_B


def host_tables():
    j = np.arange(GROUP)
    lane = np.arange(GROUP)
    q, ch = lane // 16, lane % 16
    m = 8 * q + ch % 8
    sine = ch >= 8
    m = np.where(sine & (m == 0), 64, m)
    sine = sine & (m != 64)
    angle = 2 * np.pi * (j[:, None] * m[None, :] % GROUP) / GROUP
    tc = np.where(sine[None, :], np.sin(angle), np.cos(angle)) / math.sqrt(GROUP)
    fold = np.zeros((GROUP, GROUP))
    fold[lane, m] = 1.0
    pair = (m != 0) & (m != 64)
    fold[lane[pair], GROUP - m[pair]] = np.where(sine[pair], -1.0, 1.0)
    a = np.arange(LEN_A)
    ma = np.zeros((NC, 8, LEN_A))
    for c in range(NC):
        for i in range(3):
            w = 2 * np.pi * (a * (3 * c + i) % LEN_A) / LEN_A
            ma[c, i] = np.cos(w)
            ma[c, 3 + i] = -np.sin(w)
    ma[0, 3] = np.cos(np.pi * a)
    ma = ma.reshape(NC * 8, LEN_A) / math.sqrt(LEN_A)
    lo, hi, r = np.meshgrid(np.arange(8), np.arange(3), np.arange(NR), indexing="ij")
    kb = (24 * r + 8 * hi + lo).reshape(-1)
    bp, cp = np.meshgrid(np.arange(18), np.arange(NC), indexing="ij")
    b = (18 * cp + bp).reshape(-1)
    w = 2 * np.pi * (kb[:, None] * b[None, :] % LEN_B) / LEN_B
    g = np.concatenate([np.cos(w), np.sin(w)], axis=1) / math.sqrt(LEN_B)
    small = np.zeros((8 * NC, 2 * LEN_B))
    small[:, :LEN_A] = ma
    small[:GROUP, 256:384] = tc
    small[:GROUP, 384:512] = fold
    return np.asarray(np.concatenate([g, small]), dtype=jnp.bfloat16)


TABLE = host_tables()
TILES1 = ((0, 3), (3, 5), (5, 7))
TILES3 = ((0, 2), (2, 4), (4, 7))


def swap8(x):
    lane = lax.broadcasted_iota(jnp.int32, x[0].shape, 1)
    x = list(x)
    for s in (4, 2, 1):
        shift = 16 * s
        bit = (lane & shift) != 0
        for i in range(8):
            if i & s:
                continue
            a, b = x[i], x[i + s]
            turned = pltpu.roll(a, GROUP - shift, 1)
            if b is None:
                x[i], x[i + s] = jnp.where(bit, 0.0, a), jnp.where(bit, 0.0, turned)
            else:
                x[i], x[i + s] = jnp.where(bit, pltpu.roll(b, shift, 1), a), jnp.where(bit, b, turned)
    return x


def kernel(
    tok, gain, w_in, w_out, table, out,
    xb, gn, xs, wi, wo, wf, small, gg, ma, mp, tb, s1, r1, zr, zb, sb, rb, fb,
    rr, ii, cs, sn, dd, m3, s3, r3, f3, lh, acc,
    load_sem, send1, recv1, send2, recv2, send3, recv3,
):
    row, col = lax.axis_index("row"), lax.axis_index("col")

    loads = [
        pltpu.make_async_copy(src, dst, load_sem.at[n])
        for n, (src, dst) in enumerate(
            [
                (tok, xb),
                (gain, gn),
                *[(w_in.at[pl.ds(256 * k, 256)], wi.at[pl.ds(256 * k, 256)]) for k in range(8)],
                (table.at[LEN_B:, 0:512], small),
                (table.at[0:LEN_B], gg),
                (w_out, wo),
            ]
        )
    ]
    for load in loads[:11]:
        load.start()

    barrier = pltpu.get_barrier_semaphore()

    def both_ways(me, n, act):
        act(jnp.where(me >= n // 2, me - n // 2, me + n // 2))

        def one(k, carry):
            d = n // 2 - 1 - k
            up, down = me + d, me - d
            act(jnp.where(up >= n, up - n, up))
            act(jnp.where(down < 0, down + n, down))
            return carry

        lax.fori_loop(0, n // 2 - 1, one, 0)

    def greet(axis):
        return lambda peer: pl.semaphore_signal(barrier, inc=1, device_id={axis: peer}, device_id_type=MESH)

    both_ways(row, NR, greet("row"))
    both_ways(col, NC, greet("col"))

    def send_all(src, dst, ssem, rsem, axis, me, n, first, last):
        tiles = pl.ds(first, last - first)

        def one(dest):
            pltpu.make_async_remote_copy(
                src.at[dest, tiles], dst.at[me, tiles], ssem, rsem, device_id={axis: dest}, device_id_type=MESH
            ).start()

        both_ways(me, n, one)
        dst[me, first:last] = src[me, first:last]

    def wait_all(buffer, sem, n, first, last):
        part = buffer.at[pl.ds(0, n - 1), pl.ds(first, last - first)]
        pltpu.make_async_copy(part, part, sem).wait()

    loads[0].wait()
    loads[1].wait()
    scale = gn[...].astype(F32).reshape(1, D)

    def norm(n, carry):
        x = xb[pl.ds(2 * n, 2)].astype(F32).reshape(16, D)
        y = x * lax.rsqrt(jnp.mean(x * x, axis=-1, keepdims=True) + NORM_EPS) * scale
        xs[pl.ds(pl.multiple_of(16 * n, 16), 16), :] = y.astype(BF16)
        return carry

    lax.fori_loop(0, 9, norm, 0, unroll=True)
    for k in range(4):
        at = slice(512 * k, 512 * (k + 1))
        loads[2 + 2 * k].wait()
        loads[3 + 2 * k].wait()
        part = jnp.dot(xs[:, at], wi[at, :], preferred_element_type=F32)
        if k:
            part = part + ma[...]
        if k < 3:
            ma[...] = part
        else:
            mp[...] = part.astype(BF16)
    loads[10].wait()
    loads[11].start()
    loads[12].start()
    for g in range(GROUPS):
        o, t = g // 3, g % 3
        values = jnp.dot(mp[:, 128 * g : 128 * (g + 1)], small[0:GROUP, 256:384], preferred_element_type=F32)
        tb[t, :, 8 * o : 8 * (o + 1), :] = values.reshape(18, 8, GROUP)

    def place(moved, tile):
        for q in range(8):
            for o in range(3):
                s1[8 * o + q, tile] = moved[q][8 * o : 8 * (o + 1)].astype(BF16)

    for t in range(3):
        first, last = TILES1[t]
        for hi in range(2):
            place(swap8([tb[t, 8 * hi + n] for n in range(8)]), first + hi)
        if t == 0:
            place(swap8([tb[n // 2, 16 + n % 2] if n < 6 else None for n in range(8)]), 2)
            pl.semaphore_wait(barrier, NR + NC - 2)
        send_all(s1, r1, send1.at[t], recv1.at[t], "row", row, NR, first, last)

    shape = (LEN_B, GROUP)
    line = lax.broadcasted_iota(jnp.int32, shape, 0)
    lane = lax.broadcasted_iota(jnp.int32, shape, 1)
    position = (18 * (line & 31) + (line >> 5)).astype(F32)
    sine = ((lane & 8) != 0) & jnp.logical_not((lax.rem(row, 8) == 0) & ((lane & 15) == 8))
    offset = jnp.where(sine, 0.5 * math.pi, 0.0).astype(F32)
    i = lane >> 4
    frequency = jnp.where(i < 3, 3 * col + i, LEN_A - (3 * col + i - 3))
    frequency = jnp.where((i == 3) & (col == 0), LEN_A // 2, frequency).astype(F32)
    angle = position * frequency * (2.0 * math.pi / POSITIONS) + offset
    cs[...] = jnp.cos(angle)
    sn[...] = jnp.sin(angle)
    for n in (54, 55):
        m3[pl.ds(n, NR, stride=56), :] = jnp.zeros((NR, GROUP), F32)

    def turn(x, shift):
        return pltpu.roll(x, shift % GROUP, 1) if shift % GROUP else x

    for t in range(3):
        first, last = TILES1[t]
        wait_all(r1, recv1.at[t], NR, first, last)
        arrived = [r1[:, n].astype(F32).reshape(LEN_A, GROUP) for n in range(first, last)]
        arrived = jnp.concatenate(arrived, axis=1).astype(BF16)
        turned = jnp.dot(small[:, 0:LEN_A], arrived, preferred_element_type=F32)
        for n in range(2):
            zb[pl.ds(n, 8 * NC, stride=2), :] = turned[:, 128 * n : 128 * (n + 1)]
        if t == 0:
            zr[...] = turned[:, 256:384]
        left = [zr[pl.ds(n, NC, stride=8), :] for n in range(6)]
        block = lax.broadcasted_iota(jnp.int32, (NC, GROUP), 1) >> 5
        for half, slots in ((0, (0, 1, 2, 3)), (1, (4, 5))):
            line = jnp.zeros((NC, GROUP), F32)
            for n in slots:
                line = jnp.where(block == n % 4, turn(left[n], 32 * (n % 4 - t)), line)
            zb[pl.ds(12 + half, NC, stride=16), :] = line
        sb[t] = zb[...].reshape(NC, 2, 8, GROUP).astype(BF16)
        send_all(sb.at[t], rb.at[t], send2.at[t], recv2.at[t], "col", col, NC, 0, 2)

    loads[11].wait()

    inner = (col != 0).astype(F32)
    zero = jnp.zeros((NC, GROUP), F32)

    def spread(part):
        r0, r1_, r2_, i0, i1, i2 = [part(n) for n in range(6)]
        mirrored = jnp.where(col == 0, i0, r0)
        i0 = i0 * inner
        real = swap8([r0, r1_, r2_, mirrored, r1_, r2_, None, None])
        imag = swap8([i0, i1, i2, -i0, -i1, -i2, None, None])
        return real, imag

    granule = lax.broadcasted_iota(jnp.int32, (NC, GROUP), 1) >> 4

    def gather(picks):
        tile = zero
        for n, (x, k, f) in enumerate(picks):
            value = turn(x, 16 * (n - k))
            tile = jnp.where(granule == n, value if f is None else value * f, tile)
        return tile

    for t in range(3):
        wait_all(rb.at[t], recv2.at[t], NC, 0, 2)
        fb[...] = rb[t].astype(F32).reshape(NC * 16, GROUP)
        x, y = fb[pl.ds(12, NC, stride=16), :], fb[pl.ds(13, NC, stride=16), :]
        for b2 in range(2):
            at = slice(32 * (16 + b2), 32 * (17 + b2))
            i0, i1, i2 = (x, 6 + b2), (y, b2), (y, 2 + b2)
            r0, r1_, r2_ = [(x, 2 * n + b2, None) for n in range(3)]
            tile = gather([r0, r1_, r2_, r0, r1_, r2_])
            rr[t, at, :] = jnp.where((granule == 3) & (col == 0), turn(x, 16 * (3 - i0[1])), tile)
            ii[t, at, :] = gather(
                [(*i0, inner), (*i1, None), (*i2, None), (*i0, -inner), (*i1, -1.0), (*i2, -1.0)]
            )
        for hi in range(2):
            real, imag = spread(lambda n: fb[pl.ds(2 * n + hi, NC, stride=16), :])
            for n in range(8):
                at = slice(32 * (8 * hi + n), 32 * (8 * hi + n + 1))
                rr[t, at, :] = real[n]
                ii[t, at, :] = imag[n]
        dd[0:LEN_B, :] = (rr[t] * cs[...] + ii[t] * sn[...]).astype(BF16)
        dd[LEN_B : 2 * LEN_B, :] = (ii[t] * cs[...] - rr[t] * sn[...]).astype(BF16)
        result = jnp.dot(gg[...], dd[...], preferred_element_type=F32)
        moved = swap8([result[72 * n : 72 * (n + 1)] for n in range(8)])
        for i in range(6):
            for hi in range(3):
                m3[pl.ds(18 * t + 3 * i + hi, NR, stride=56), :] = moved[i][24 * hi : 24 * (hi + 1)]
        first, last = TILES3[t]
        s3[:, first:last] = m3.reshape(NR, 7, 8, GROUP)[:, first:last].astype(BF16)
        send_all(s3, r3, send3.at[t], recv3.at[t], "row", row, NR, first, last)

    def take(first, last):
        f3.reshape(NR, 7, 8, GROUP)[:, first:last] = r3[:, first:last].astype(F32)

    def project(chunks):
        values = []
        for t in chunks:
            for o in range(3):
                moved = swap8([f3[pl.ds((8 * o + q) * 56 + 18 * t, 18), :] for q in range(8)])
                for n in range(8):
                    lh[3 * t + o, pl.ds(n, 18, stride=8), :] = moved[n]
                values.append(lh[3 * t + o])
        values = jnp.concatenate(values, axis=1).astype(BF16)
        lines = slice(384 * chunks[0], 384 * (chunks[-1] + 1))
        for n in range(D // 512):
            at = slice(512 * n, 512 * (n + 1))
            part = jnp.dot(values, wf[lines, at], preferred_element_type=F32)
            if chunks[0]:
                out[:, at] = (part + acc[:, at]).astype(BF16)
            else:
                acc[:, at] = part

    loads[12].wait()
    for t in range(3):
        for o in range(3):
            source, target = 128 * (3 * o + t), 128 * (3 * t + o)
            wf[target : target + 128, :] = jnp.dot(
                small[0:GROUP, 384:512], wo[source : source + 128, :], preferred_element_type=F32
            ).astype(BF16)
    wait_all(r3, recv3.at[0], NR, *TILES3[0])
    wait_all(r3, recv3.at[1], NR, *TILES3[1])
    take(0, 4)
    project((0,))
    wait_all(r3, recv3.at[2], NR, *TILES3[2])
    take(4, 7)
    project((1, 2))

    for t in range(3):
        wait_all(s1, send1.at[t], NR, *TILES1[t])
        wait_all(sb.at[t], send2.at[t], NC, 0, 2)
        wait_all(s3, send3.at[t], NR, *TILES3[t])


def shards(tokens, norm_gain, w_in, w_out):
    vm = pltpu.VMEM
    dma = pltpu.SemaphoreType.DMA
    operands = tokens.transpose(1, 0, 2), norm_gain, w_in, w_out, jnp.asarray(TABLE)
    out = pl.pallas_call(
        kernel,
        out_shape=jax.ShapeDtypeStruct((144, D), BF16),
        in_specs=[pl.BlockSpec(memory_space=pl.ANY)] * 5,
        out_specs=pl.BlockSpec(memory_space=vm),
        scratch_shapes=[
            vm((18, 8, D), BF16),
            vm((D,), BF16),
            vm((144, D), BF16),
            vm((D, F), BF16),
            vm((F, D), BF16),
            vm((F, D), BF16),
            vm((8 * NC, 512), BF16),
            vm((LEN_B, 2 * LEN_B), BF16),
            vm((144, F), F32),
            vm((144, F), BF16),
            vm((3, 18, 24, GROUP), F32),
            vm((NR, 7, 8, GROUP), BF16),
            vm((NR, 7, 8, GROUP), BF16),
            vm((NC * 8, GROUP), F32),
            vm((NC * 16, GROUP), F32),
            vm((3, NC, 2, 8, GROUP), BF16),
            vm((3, NC, 2, 8, GROUP), BF16),
            vm((NC * 16, GROUP), F32),
            vm((3, LEN_B, GROUP), F32),
            vm((3, LEN_B, GROUP), F32),
            vm((LEN_B, GROUP), F32),
            vm((LEN_B, GROUP), F32),
            vm((2 * LEN_B, GROUP), BF16),
            vm((NR * 56, GROUP), F32),
            vm((NR, 7, 8, GROUP), BF16),
            vm((NR, 7, 8, GROUP), BF16),
            vm((NR * 56, GROUP), F32),
            vm((9, 144, GROUP), F32),
            vm((144, D), F32),
            dma((13,)),
            dma((3,)),
            dma((3,)),
            dma((3,)),
            dma((3,)),
            dma((3,)),
            dma((3,)),
        ],
        compiler_params=pltpu.CompilerParams(
            collective_id=0, has_side_effects=True, vmem_limit_bytes=50 * 1024 * 1024
        ),
    )(*[pltpu.with_memory_space_constraint(x, pltpu.HBM) for x in operands])
    return out.reshape(6, 3, 8, D).transpose(1, 2, 0, 3).reshape(24, 6, D)


def solution(mesh):
    in_specs = (P("row", "col", None), P(), P(), P())
    out_specs = P("row", "col", None)
    return jax.shard_map(shards, mesh=mesh, in_specs=in_specs, out_specs=out_specs, check_vma=False)
```
